32 devices in a mesh: grp: 2 (over x), ep: 8 (over z, y), tp: 2 (over core).
Axes of the slice: x: 2, y: 2, z: 4, core: 2. Of those that a mesh axis runs over, the one named last changes fastest.
Arguments:
- tokens: bfloat16 [1024, 2048], P(('grp', 'ep')), parts along dimension 0, may hold values from -6 to 6
- norm_gain: bfloat16 [2048], replicated, may hold values from 0.099609375 to 1.8984375
- routes: int32 [1024, 4], P(('grp', 'ep')), parts along dimension 0, may hold values from 0 to 7, all different within a row; in each aligned block of 64 rows (0 to 63, 64 to 127, ...) at most 64 rows name the same one
- route_weights: float32 [1024, 4], P(('grp', 'ep')), parts along dimension 0, may hold values from 0.2 to 1
- gate_experts: bfloat16 [8, 2048, 512], P('ep', None, 'tp'), may hold values from -0.125 to 0.125
- up_experts: bfloat16 [8, 2048, 512], P('ep', None, 'tp'), may hold values from -0.125 to 0.125
- down_experts: bfloat16 [8, 512, 2048], P('ep', 'tp'), may hold values from -0.25 to 0.25
- shared_gate: bfloat16 [2048, 512], P(None, 'tp'), may hold values from -0.125 to 0.125
- shared_up: bfloat16 [2048, 512], P(None, 'tp'), may hold values from -0.125 to 0.125
- shared_down: bfloat16 [512, 2048], P('tp'), may hold values from -0.25 to 0.25
- out_gain: bfloat16 [2048], P('tp'), may hold values from 0.099609375 to 1.8984375
Outputs:
- result: bfloat16 [1024, 2048], P(('grp', 'ep'), 'tp'), parts along dimension 0
The draws below stay inside these ranges and needn't reach their ends.
There are 2 independent parts, one for each index of `grp`. The reference program is written for one: setup_inputs(seed, part) draws one part's arguments, and reference() takes and returns one part's arrays. A program takes and returns all parts, laid end to end along the dimension named above; an argument that names none is the same for every part. Nothing has to cross between parts.
Inputs may be any that keep to these rules, and one draw needn't show every extreme that they name: `routes`: each row names 4 different experts. Among the 64 rows of one index of ep at most 64 name the same expert, and in every draw some expert is named by exactly 64 rows of some index.
All inputs are finite; a program needn't handle non-finite values.
Results may differ from the reference program's by a relative error of at most 0.0077.
Values may be sent and summed in bfloat16 or wider, within the bound.
A program may use at most 64 MiB of HBM per device.

```python
import math
import jax
import jax.numpy as jnp
import numpy as np
from jax import lax

D = 2048
FF = 512
SF = 512
TOP_K = 4
TOK_DEV = 64
EXPERTS = 8
CAP = 64
TOKENS = 512
N_TP = 2


def shard_levels(stream_key, extent, cuts, low, largest):
    def one(axis_at, blocks):
        heights = jax.random.uniform(jax.random.fold_in(jax.random.fold_in(stream_key, 6), axis_at), (blocks,), jnp.float32, low / len(cuts), largest / len(cuts))
        return jnp.repeat(jnp.exp(heights), extent[axis_at] // blocks).reshape((-1,) + (1,) * (len(extent) - axis_at - 1))

    level = one(*cuts[0])
    for cut in cuts[1:]:
        level = level * one(*cut)
    return level


def shared_out(own_key, own, number, rows, amount, top, limit, lean):
    sequence = jax.random.permutation(own_key, amount)
    packed, usual = shares(amount, rows * top, limit, lean, True), shares(amount, rows * top, limit, lean, False)
    places = jnp.arange(amount)

    def named(tallies, turn):
        used = int((tallies > 0).sum())
        fixed = max(1, used // 4)
        moved = fixed + (places - fixed + turn * (used - fixed)) % max(1, amount - fixed)
        return jnp.zeros((amount,), jnp.int32).at[sequence[jnp.where(places < fixed, places, moved)]].set(jnp.asarray(tallies, jnp.int32))

    tallies = jnp.where(number % 4 == 0, named(packed, number // 4), named(usual, number - number // 4 - 1))
    mixed = jax.random.permutation(jax.random.fold_in(own, 3), amount)
    giver, receiver = mixed[0:amount // 2 * 2:2], mixed[1:amount // 2 * 2:2]
    slack = jnp.minimum(tallies[giver] - 1, limit - tallies[receiver]) // 2
    slack = jnp.where((giver == sequence[0]) | (receiver == sequence[0]) | (tallies[receiver] == 0), 0, jnp.maximum(slack, 0))
    moved = jax.random.randint(jax.random.fold_in(own, 4), (amount // 2,), 0, 1 << 20) % (slack + 1)
    tallies = tallies.at[giver].add(-moved).at[receiver].add(moved)
    items = jnp.searchsorted(jnp.cumsum(tallies), jnp.arange(rows * top), side="right").astype(jnp.int32)
    listing = items.reshape(top, rows).T
    listing = listing[jax.random.permutation(jax.random.fold_in(own, 1), rows)]
    turn = jax.random.randint(jax.random.fold_in(own, 2), (rows, 1), 0, top)
    return jnp.take_along_axis(listing, (jnp.arange(top)[None, :] + turn) % top, axis=1)


def shares(count, total, bound, skew, full):
    loads = [(1 << 20) // math.isqrt(standing ** skew) + 1 for standing in range(1, count + 1)]
    largest = bound if full else min(bound, max(-(-total // count), total * loads[0] // sum(loads)))
    least = 1 if total - largest >= count - 1 else 0
    counts, spare = [largest] + [least] * (count - 1), total - largest - least * (count - 1)
    while spare > 0:
        candidates = [i for i in range(1, count) if counts[i] < largest] or [i for i in range(1, count) if counts[i] < bound]
        pool, left = sum([loads[i] for i in candidates]), spare
        for i in candidates:
            more = min(bound - counts[i], max(1, left * loads[i] // pool), spare)
            counts[i] = counts[i] + more
            spare = spare - more
    return np.array(counts)


def bell_draw(key, shape, deviation, most, shards=(), kind=jnp.bfloat16):
    result = jax.random.normal(key, shape, jnp.float32) * deviation
    if len(shards) > 0:
        result = shard_levels(key, shape, shards, -0.22, 0.18) * result
    return jnp.clip(result, min=-most, max=most).astype(kind)


def setup_inputs(seed: int = 0, part: int = 0) -> dict:
    keys = jax.random.split(jax.random.key(seed), 12)
    part_keys = jax.random.split(jax.random.fold_in(keys[11], part), 12)
    tokens = bell_draw(part_keys[0], (TOKENS, D), 1.0, 6.0, ((0, 8),))
    norm_gain = jnp.clip(1.0 + 0.18 * jax.random.normal(keys[1], (D,), jnp.float32), 0.099609375, 1.8984375).astype(jnp.bfloat16)
    routes_keys = jax.random.split(jax.random.fold_in(part_keys[2], 1), TOKENS // TOK_DEV)
    routes_turns = jax.random.permutation(jax.random.fold_in(part_keys[2], 3), TOKENS // TOK_DEV)
    routes = jax.vmap(lambda own, number: shared_out(jax.random.fold_in(part_keys[2], 2), own, number, TOK_DEV, EXPERTS, TOP_K, CAP, 2))(routes_keys, routes_turns).reshape((TOKENS, TOP_K))
    route_weights = jnp.clip(0.2 + 0.8 * jax.random.uniform(part_keys[3], (TOKENS, TOP_K), jnp.float32) ** shard_levels(part_keys[3], (TOKENS, TOP_K), ((0, 8),), -0.2, 0.2), 0.2, 1.0)
    gate_experts = bell_draw(keys[4], (EXPERTS, D, FF), D ** -0.5, 0.125, ((0, 8), (2, 2)))
    up_experts = bell_draw(keys[5], (EXPERTS, D, FF), D ** -0.5, 0.125, ((0, 8), (2, 2)))
    down_experts = bell_draw(keys[6], (EXPERTS, FF, D), FF ** -0.5, 0.25, ((0, 8), (1, 2)))
    shared_gate = bell_draw(keys[7], (D, SF), D ** -0.5, 0.125, ((1, 2),))
    shared_up = bell_draw(keys[8], (D, SF), D ** -0.5, 0.125, ((1, 2),))
    shared_down = bell_draw(keys[9], (SF, D), SF ** -0.5, 0.25, ((0, 2),))
    out_gain = jnp.clip(1.0 + 0.18 * jax.random.normal(keys[10], (D,), jnp.float32), 0.099609375, 1.8984375).astype(jnp.bfloat16)
    return dict(tokens=tokens, norm_gain=norm_gain, routes=routes, route_weights=route_weights, gate_experts=gate_experts, up_experts=up_experts, down_experts=down_experts, shared_gate=shared_gate, shared_up=shared_up, shared_down=shared_down, out_gain=out_gain)


EPS = 1e-06

def block_sum(activated, down_w):
    out_rows = activated.shape[0]
    block_width = activated.shape[1] // N_TP
    pieces = jnp.einsum('rtf,tfd->rtd', activated.reshape(out_rows, N_TP, block_width).astype(jnp.float32), down_w.reshape(N_TP, block_width, -1).astype(jnp.float32))
    rounded = lax.optimization_barrier(pieces.astype(jnp.bfloat16))
    return lax.optimization_barrier(jnp.sum(rounded.astype(jnp.float32), axis=1)).astype(jnp.bfloat16)

def swiglu_rows(normed, gate_w, up_w, down_w):
    gate_value = jnp.dot(normed, gate_w, preferred_element_type=jnp.float32)
    up_value = jnp.dot(normed, up_w, preferred_element_type=jnp.float32)
    activated = (jax.nn.silu(gate_value) * up_value).astype(jnp.bfloat16)
    return block_sum(activated, down_w)

def reference(tokens, norm_gain, routes, route_weights, gate_experts, up_experts, down_experts, shared_gate, shared_up, shared_down, out_gain):
    wide_tokens = tokens.astype(jnp.float32)
    normed = (wide_tokens * lax.rsqrt(lax.optimization_barrier(jnp.mean(wide_tokens * wide_tokens, axis=1, keepdims=True)) + EPS) * norm_gain.astype(jnp.float32)).astype(jnp.bfloat16)
    expert_total = gate_experts.shape[0]

    def expert_step(accum, inputs):
        gate_w, up_w, down_w, expert_id = inputs
        out_rows = swiglu_rows(normed, gate_w, up_w, down_w).astype(jnp.float32)
        weight_sum = lax.optimization_barrier(jnp.sum(jnp.where(routes == expert_id, route_weights, 0.0), axis=1))
        return (accum + weight_sum[:, None] * out_rows, None)
    start = jnp.zeros((tokens.shape[0], tokens.shape[1]), jnp.float32)
    routed, _ = lax.scan(expert_step, start, (gate_experts, up_experts, down_experts, jnp.arange(expert_total, dtype=jnp.int32)))
    shared = swiglu_rows(normed, shared_gate, shared_up, shared_down).astype(jnp.float32)
    mixed = shared + routed
    inverse = lax.rsqrt(lax.optimization_barrier(jnp.mean(mixed * mixed, axis=1, keepdims=True)) + EPS)
    return (mixed * inverse * out_gain.astype(jnp.float32)).astype(jnp.bfloat16)
```

```python
import functools

import jax
import jax.numpy as jnp
from jax import lax
from jax.experimental import pallas as pl
from jax.experimental.pallas import tpu as pltpu
from jax.sharding import PartitionSpec as P

EPS = 1e-06
MESH = pl.DeviceIdType.MESH
LANES = 128
HALF_LANES = LANES // 2


def xor(a, b, size):
    total, bit = 0, 1
    while bit < size:
        total = total + ((a // bit + b // bit) % 2) * bit
        bit *= 2
    return total


def kernel(
    ep,
    tokens_ref,
    norm_gain_ref,
    routes_ref,
    weights_ref,
    gate_hbm,
    up_hbm,
    down_hbm,
    sgate_hbm,
    sup_hbm,
    sdown_hbm,
    out_gain_ref,
    result_ref,
    gathered,
    gate,
    up,
    down,
    sgate,
    sup,
    sdown,
    kept,
    shared_kept,
    core_out,
    core_in,
    score_out,
    score_in,
    y_out,
    y_in,
    z_out,
    z_in,
    local_sum,
    sq_out,
    sq_in,
    load_sem,
    z_send,
    z_recv,
    y_send,
    y_recv,
    cz_send,
    cz_recv,
    cy_send,
    cy_recv,
    co_send,
    co_recv,
    yo_send,
    yo_recv,
    zo_send,
    zo_recv,
    sq_send,
    sq_recv,
):
    zs = ep // 2
    rows, width = tokens_ref.shape
    half_rows, half_width = rows // 2, width // 2
    me = lax.axis_index("ep")
    core = lax.axis_index("tp")
    z, y = me // 2, me % 2
    zz = [xor(z, s, zs) for s in range(zs)]
    sibling = {"tp": 1 - core}
    across = {"ep": z * 2 + (1 - y)}
    along = [{"ep": zz[s] * 2 + y} for s in range(zs)]

    loads = []
    for i, (src, dst) in enumerate(
        [
            (sgate_hbm, sgate),
            (sup_hbm, sup),
            (sdown_hbm, sdown),
            (gate_hbm.at[0], gate),
            (up_hbm.at[0], up),
            (down_hbm.at[0], down),
        ]
    ):
        copy = pltpu.make_async_copy(src, dst, load_sem.at[i])
        copy.start()
        loads.append(copy)

    barrier = pltpu.get_barrier_semaphore()
    peers = [sibling, across] + along[1:]
    for peer in peers:
        pl.semaphore_signal(barrier, inc=1, device_id=peer, device_id_type=MESH)

    wide = tokens_ref[...].astype(jnp.float32)
    scale = lax.rsqrt(jnp.mean(wide * wide, axis=1, keepdims=True) + EPS)
    gain = norm_gain_ref[...].astype(jnp.float32)
    gathered[me, :, :width] = (wide * scale * gain).astype(jnp.bfloat16)
    lane = lax.broadcasted_iota(jnp.int32, (rows, LANES), 1)
    chosen = jnp.zeros((rows, LANES), jnp.float32)
    for k in range(routes_ref.shape[1]):
        hit = routes_ref[:, k : k + 1] == lane % HALF_LANES
        chosen = chosen + jnp.where(hit, weights_ref[:, k : k + 1], 0.0)
    high = chosen.astype(jnp.bfloat16).astype(jnp.float32)
    gathered[me, :, width:] = jnp.where(lane < HALF_LANES, high, chosen - high).astype(
        jnp.bfloat16
    )

    pl.semaphore_wait(barrier, len(peers))

    my_rows = pl.ds(pl.multiple_of(core * half_rows, half_rows), half_rows)
    other_rows = pl.ds(pl.multiple_of((1 - core) * half_rows, half_rows), half_rows)
    my_cols = pl.ds(pl.multiple_of(core * half_width, half_width), half_width)
    other_cols = pl.ds(pl.multiple_of((1 - core) * half_width, half_width), half_width)

    sent = []

    def send(src, dst, send_sem, recv_sem, target):
        copy = pltpu.make_async_remote_copy(
            src_ref=src,
            dst_ref=dst,
            send_sem=send_sem,
            recv_sem=recv_sem,
            device_id=target,
            device_id_type=MESH,
        )
        copy.start()
        sent.append(copy)
        return copy

    def arrived(ref, send_sem, recv_sem, target):
        pltpu.make_async_remote_copy(
            src_ref=ref,
            dst_ref=ref,
            send_sem=send_sem,
            recv_sem=recv_sem,
            device_id=target,
            device_id_type=MESH,
        ).wait_recv()

    own = gathered.at[me, my_rows]
    send(own, own, y_send.at[0], y_recv.at[0], across)
    for s in range(1, zs):
        send(own, own, z_send.at[s], z_recv.at[s], along[s])

    def take_z(s):
        block = gathered.at[zz[s] * 2 + y, my_rows]
        arrived(block, z_send.at[s], z_recv.at[s], along[s])
        send(block, block, y_send.at[s], y_recv.at[s], across)
        send(block, block, cz_send.at[s], cz_recv.at[s], sibling)

    def take_y(s):
        block = gathered.at[zz[s] * 2 + (1 - y), my_rows]
        arrived(block, y_send.at[s], y_recv.at[s], across)
        send(block, block, cy_send.at[s], cy_recv.at[s], sibling)

    def take_core(s):
        if s > 0:
            block = gathered.at[zz[s] * 2 + y, other_rows]
            arrived(block, cz_send.at[s], cz_recv.at[s], sibling)
        block = gathered.at[zz[s] * 2 + (1 - y), other_rows]
        arrived(block, cy_send.at[s], cy_recv.at[s], sibling)

    def swiglu(x, gate_w, up_w):
        g = jnp.dot(x, gate_w[...], preferred_element_type=jnp.float32)
        u = jnp.dot(x, up_w[...], preferred_element_type=jnp.float32)
        return (g / (1.0 + jnp.exp(-g)) * u).astype(jnp.bfloat16)

    def experts(s):
        pair = gathered.at[pl.ds(zz[s] * 2, 2)]
        x = pair[:, :, :width].reshape(2 * rows, width)
        act = swiglu(x, gate, up)
        core_out[s] = jnp.dot(
            act, down[:, other_cols], preferred_element_type=jnp.float32
        ).astype(jnp.bfloat16)
        send(core_out.at[s], core_in.at[s], co_send.at[s], co_recv.at[s], sibling)
        kept[s] = jnp.dot(act, down[:, my_cols], preferred_element_type=jnp.float32)

    def weight_of(block):
        spread = gathered[block, :, width:].astype(jnp.float32)
        return jnp.sum(
            jnp.where(lane % HALF_LANES == me, spread, 0.0), axis=1, keepdims=True
        )

    def combine(s):
        arrived(core_in.at[s], co_send.at[s], co_recv.at[s], sibling)
        theirs = pl.ds(pl.multiple_of((1 - y) * rows, rows), rows)
        value = kept[s, theirs] + core_in[s, theirs].astype(jnp.float32)
        y_out[s] = (value * weight_of(zz[s] * 2 + (1 - y))).astype(jnp.bfloat16)
        send(y_out.at[s], y_in.at[s], yo_send.at[s], yo_recv.at[s], across)

    def finish(s):
        mine = pl.ds(pl.multiple_of(y * rows, rows), rows)
        value = kept[s, mine] + core_in[s, mine].astype(jnp.float32)
        value = value * weight_of(zz[s] * 2 + y)
        arrived(y_in.at[s], yo_send.at[s], yo_recv.at[s], across)
        value = value + y_in[s].astype(jnp.float32)
        if s == 0:
            local_sum[...] = value
        else:
            z_out[s] = value.astype(jnp.bfloat16)
            send(z_out.at[s], z_in.at[s], zo_send.at[s], zo_recv.at[s], along[s])

    for i in range(3):
        loads[i].wait()
    act = swiglu(gathered[me, :, :width], sgate, sup)
    score_out[...] = jnp.dot(
        act, sdown[:, other_cols], preferred_element_type=jnp.float32
    ).astype(jnp.bfloat16)
    send(score_out, score_in, co_send.at[zs], co_recv.at[zs], sibling)
    shared_kept[...] = jnp.dot(act, sdown[:, my_cols], preferred_element_type=jnp.float32)
    for i in range(3, 6):
        loads[i].wait()

    for s in range(zs + 2):
        if s < zs:
            if s + 1 < zs:
                if s == 0:
                    take_y(0)
                take_z(s + 1)
            if s > 0 or zs == 1:
                take_y(s)
            take_core(s)
            experts(s)
        if 1 <= s <= zs:
            combine(s - 1)
        if s >= 2:
            finish(s - 2)

    arrived(score_in, co_send.at[zs], co_recv.at[zs], sibling)
    mixed = local_sum[...] + (shared_kept[...] + score_in[...].astype(jnp.float32))
    for s in range(1, zs):
        arrived(z_in.at[s], zo_send.at[s], zo_recv.at[s], along[s])
        mixed = mixed + z_in[s].astype(jnp.float32)
    local_sum[...] = mixed
    squares = jnp.sum(mixed * mixed, axis=1, keepdims=True)
    sq_out[...] = jnp.broadcast_to(squares, sq_out.shape)
    send(sq_out, sq_in, sq_send, sq_recv, sibling)
    arrived(sq_in, sq_send, sq_recv, sibling)
    inverse = lax.rsqrt((squares + sq_in[:, :1]) / width + EPS)
    result_ref[...] = (
        local_sum[...] * inverse * out_gain_ref[...].astype(jnp.float32)
    ).astype(jnp.bfloat16)
    for copy in sent:
        copy.wait_send()


def per_device(tokens, norm_gain, routes, route_weights, gate, up, down, sgate, sup, sdown, out_gain):
    ep = lax.axis_size("ep")
    zs = ep // 2
    rows, width = tokens.shape
    hidden, shidden = gate.shape[2], sgate.shape[1]
    half = width // 2
    bf, f32 = jnp.bfloat16, jnp.float32
    vmem = pl.BlockSpec(memory_space=pltpu.VMEM)
    hbm = pl.BlockSpec(memory_space=pl.ANY)
    dma = pltpu.SemaphoreType.DMA
    flops = 6 * rows * width * (ep * hidden + shidden)
    return pl.pallas_call(
        functools.partial(kernel, ep),
        out_shape=jax.ShapeDtypeStruct((rows, half), bf),
        in_specs=[vmem] * 4 + [hbm] * 6 + [vmem],
        out_specs=vmem,
        scratch_shapes=[
            pltpu.VMEM((ep, rows, width + LANES), bf),
            pltpu.VMEM((width, hidden), bf),
            pltpu.VMEM((width, hidden), bf),
            pltpu.VMEM((hidden, width), bf),
            pltpu.VMEM((width, shidden), bf),
            pltpu.VMEM((width, shidden), bf),
            pltpu.VMEM((shidden, width), bf),
            pltpu.VMEM((zs, 2 * rows, half), f32),
            pltpu.VMEM((rows, half), f32),
            pltpu.VMEM((zs, 2 * rows, half), bf),
            pltpu.VMEM((zs, 2 * rows, half), bf),
            pltpu.VMEM((rows, half), bf),
            pltpu.VMEM((rows, half), bf),
            pltpu.VMEM((zs, rows, half), bf),
            pltpu.VMEM((zs, rows, half), bf),
            pltpu.VMEM((zs, rows, half), bf),
            pltpu.VMEM((zs, rows, half), bf),
            pltpu.VMEM((rows, half), f32),
            pltpu.VMEM((rows, LANES), f32),
            pltpu.VMEM((rows, LANES), f32),
            dma((6,)),
            dma((zs,)),
            dma((zs,)),
            dma((zs,)),
            dma((zs,)),
            dma((zs,)),
            dma((zs,)),
            dma((zs,)),
            dma((zs,)),
            dma((zs + 1,)),
            dma((zs + 1,)),
            dma((zs,)),
            dma((zs,)),
            dma((zs,)),
            dma((zs,)),
            dma,
            dma,
        ],
        compiler_params=pltpu.CompilerParams(
            collective_id=0, has_side_effects=True, vmem_limit_bytes=60 * 1024 * 1024
        ),
        cost_estimate=pl.CostEstimate(
            flops=flops, bytes_accessed=6 * width * (hidden + shidden), transcendentals=0
        ),
    )(
        tokens,
        norm_gain.reshape(1, -1),
        routes,
        route_weights,
        gate,
        up,
        down,
        sgate,
        sup,
        sdown,
        out_gain.reshape(1, -1),
    )


def solution(mesh):
    in_specs = (
        P(("grp", "ep"), None),
        P(),
        P(("grp", "ep"), None),
        P(("grp", "ep"), None),
        P("ep", None, "tp"),
        P("ep", None, "tp"),
        P("ep", "tp", None),
        P(None, "tp"),
        P(None, "tp"),
        P("tp", None),
        P("tp"),
    )
    out_specs = P(("grp", "ep"), "tp")
    return jax.shard_map(
        per_device, mesh=mesh, in_specs=in_specs, out_specs=out_specs, check_vma=False
    )
```

```python
import functools

import jax
import jax.numpy as jnp
from jax import lax
from jax.experimental import pallas as pl
from jax.experimental.pallas import tpu as pltpu
from jax.sharding import PartitionSpec as P

EPS = 1e-06
MESH = pl.DeviceIdType.MESH
LANES = 128
HALF_LANES = LANES // 2


PIECES = 2


def by_distance(z, zs):
    table = [sorted(range(zs), key=lambda o: (abs(o - at), -o)) for at in range(zs)]
    order = []
    for k in range(zs):
        pick = table[0][k]
        for at in range(1, zs):
            pick = jnp.where(z == at, table[at][k], pick)
        order.append(pick)
    return order


def kernel(
    ep,
    tokens_ref,
    norm_gain_ref,
    routes_ref,
    weights_ref,
    gate_hbm,
    up_hbm,
    down_hbm,
    sgate_hbm,
    sup_hbm,
    sdown_hbm,
    out_gain_ref,
    result_ref,
    gathered,
    gate,
    up,
    down,
    sgate,
    sup,
    sdown,
    kept,
    shared_kept,
    core_out,
    core_in,
    score_out,
    score_in,
    y_out,
    y_in,
    z_out,
    z_in,
    local_sum,
    sq_out,
    sq_in,
    load_sem,
    r_send,
    l_send,
    z_recv,
    y_send,
    y_recv,
    cz_send,
    cz_recv,
    cy_send,
    cy_recv,
    co_send,
    co_recv,
    yo_send,
    yo_recv,
    zo_send,
    zo_recv,
    sq_send,
    sq_recv,
):
    zs = ep // 2
    rows, width = tokens_ref.shape
    half_rows, half_width = rows // 2, width // 2
    me = lax.axis_index("ep")
    core = lax.axis_index("tp")
    z, y = me // 2, me % 2
    zz = by_distance(z, zs)
    sibling = {"tp": 1 - core}
    across = {"ep": z * 2 + (1 - y)}
    along = [{"ep": zz[s] * 2 + y} for s in range(zs)]

    loads = []
    for i, (src, dst) in enumerate(
        [
            (gate_hbm.at[0], gate),
            (up_hbm.at[0], up),
            (down_hbm.at[0], down),
            (sgate_hbm, sgate),
            (sup_hbm, sup),
            (sdown_hbm, sdown),
        ]
    ):
        copy = pltpu.make_async_copy(src, dst, load_sem.at[i])
        copy.start()
        loads.append(copy)

    barrier = pltpu.get_barrier_semaphore()
    peers = [sibling, across] + along[1:]
    for peer in peers:
        pl.semaphore_signal(barrier, inc=1, device_id=peer, device_id_type=MESH)

    wide = tokens_ref[...].astype(jnp.float32)
    scale = lax.rsqrt(jnp.mean(wide * wide, axis=1, keepdims=True) + EPS)
    gain = norm_gain_ref[...].astype(jnp.float32).reshape(1, width)
    gathered[me, :, :width] = (wide * scale * gain).astype(jnp.bfloat16)
    lane = lax.broadcasted_iota(jnp.int32, (rows, LANES), 1)
    expert = lax.broadcasted_iota(jnp.int32, (LANES, rows), 0) % HALF_LANES
    chosen = jnp.zeros((LANES, rows), jnp.float32)
    for k in range(routes_ref.shape[0]):
        hit = routes_ref[k : k + 1, :] == expert
        chosen = chosen + jnp.where(hit, weights_ref[k : k + 1, :], 0.0)
    chosen = chosen.T
    high = chosen.astype(jnp.bfloat16).astype(jnp.float32)
    gathered[me, :, width:] = jnp.where(lane < HALF_LANES, high, chosen - high).astype(
        jnp.bfloat16
    )

    pl.semaphore_wait(barrier, len(peers))

    piece = half_rows // PIECES

    def rows_of(which, q):
        return pl.ds(pl.multiple_of(which * half_rows + q * piece, piece), piece)

    my_cols = pl.ds(pl.multiple_of(core * half_width, half_width), half_width)
    other_cols = pl.ds(pl.multiple_of((1 - core) * half_width, half_width), half_width)

    sent = []

    def send(src, dst, send_sem, recv_sem, target):
        copy = pltpu.make_async_remote_copy(
            src_ref=src,
            dst_ref=dst,
            send_sem=send_sem,
            recv_sem=recv_sem,
            device_id=target,
            device_id_type=MESH,
        )
        copy.start()
        sent.append(copy)
        return copy

    def arrived(ref, send_sem, recv_sem, target):
        pltpu.make_async_remote_copy(
            src_ref=ref,
            dst_ref=ref,
            send_sem=send_sem,
            recv_sem=recv_sem,
            device_id=target,
            device_id_type=MESH,
        ).wait_recv()

    passed = []

    def pass_on(block, q, source, sends, target, when):
        copy = pltpu.make_async_remote_copy(
            src_ref=block,
            dst_ref=block,
            send_sem=sends.at[source, q],
            recv_sem=z_recv.at[source, q],
            device_id={"ep": target * 2 + y},
            device_id_type=MESH,
        )
        pl.when(when)(copy.start)
        passed.append((copy, when))

    for q in range(PIECES):
        own = gathered.at[me, rows_of(core, q)]
        pass_on(own, q, z, r_send, z + 1, z < zs - 1)
        pass_on(own, q, z, l_send, z - 1, z > 0)
        send(own, own, y_send.at[0, q], y_recv.at[0, q], across)

    def take_z(s):
        for q in range(PIECES):
            block = gathered.at[zz[s] * 2 + y, rows_of(core, q)]
            arrived(block, r_send.at[zz[s], q], z_recv.at[zz[s], q], across)
            pass_on(block, q, zz[s], r_send, z + 1, jnp.logical_and(zz[s] < z, z < zs - 1))
            pass_on(block, q, zz[s], l_send, z - 1, jnp.logical_and(zz[s] > z, z > 0))
            send(block, block, y_send.at[s, q], y_recv.at[s, q], across)
            send(block, block, cz_send.at[s, q], cz_recv.at[s, q], sibling)

    def take_y(s):
        for q in range(PIECES):
            block = gathered.at[zz[s] * 2 + (1 - y), rows_of(core, q)]
            arrived(block, y_send.at[s, q], y_recv.at[s, q], across)
            send(block, block, cy_send.at[s, q], cy_recv.at[s, q], sibling)

    def take_core(s):
        for q in range(PIECES):
            if s > 0:
                block = gathered.at[zz[s] * 2 + y, rows_of(1 - core, q)]
                arrived(block, cz_send.at[s, q], cz_recv.at[s, q], sibling)
            block = gathered.at[zz[s] * 2 + (1 - y), rows_of(1 - core, q)]
            arrived(block, cy_send.at[s, q], cy_recv.at[s, q], sibling)

    def swiglu(x, gate_w, up_w):
        g = jnp.dot(x, gate_w[...], preferred_element_type=jnp.float32)
        u = jnp.dot(x, up_w[...], preferred_element_type=jnp.float32)
        return (g / (1.0 + jnp.exp(-g)) * u).astype(jnp.bfloat16)

    def experts(s):
        pair = gathered.at[pl.ds(zz[s] * 2, 2)]
        x = pair[:, :, :width].reshape(2 * rows, width)
        act = swiglu(x, gate, up)
        core_out[s] = jnp.dot(
            act, down[:, other_cols], preferred_element_type=jnp.float32
        ).astype(jnp.bfloat16)
        send(core_out.at[s], core_in.at[s], co_send.at[s], co_recv.at[s], sibling)
        kept[s] = jnp.dot(act, down[:, my_cols], preferred_element_type=jnp.float32)

    def weight_of(block):
        spread = gathered[block, :, width:].astype(jnp.float32)
        return jnp.sum(
            jnp.where(lane % HALF_LANES == me, spread, 0.0), axis=1, keepdims=True
        )

    def combine(s):
        arrived(core_in.at[s], co_send.at[s], co_recv.at[s], sibling)
        theirs = pl.ds(pl.multiple_of((1 - y) * rows, rows), rows)
        value = kept[s, theirs] + core_in[s, theirs].astype(jnp.float32)
        y_out[s] = (value * weight_of(zz[s] * 2 + (1 - y))).astype(jnp.bfloat16)
        send(y_out.at[s], y_in.at[s], yo_send.at[s], yo_recv.at[s], across)

    def finish(s):
        mine = pl.ds(pl.multiple_of(y * rows, rows), rows)
        value = kept[s, mine] + core_in[s, mine].astype(jnp.float32)
        value = value * weight_of(zz[s] * 2 + y)
        arrived(y_in.at[s], yo_send.at[s], yo_recv.at[s], across)
        value = value + y_in[s].astype(jnp.float32)
        if s == 0:
            local_sum[...] = value
        else:
            z_out[s] = value.astype(jnp.bfloat16)
            send(z_out.at[s], z_in.at[z], zo_send.at[s], zo_recv.at[z], along[s])

    def shared_expert():
        for i in range(3, 6):
            loads[i].wait()
        act = swiglu(gathered[me, :, :width], sgate, sup)
        score_out[...] = jnp.dot(
            act, sdown[:, other_cols], preferred_element_type=jnp.float32
        ).astype(jnp.bfloat16)
        send(score_out, score_in, co_send.at[zs], co_recv.at[zs], sibling)
        shared_kept[...] = jnp.dot(act, sdown[:, my_cols], preferred_element_type=jnp.float32)

    ahead = 2
    for s in range(1, min(1 + ahead, zs)):
        take_z(s)
    for s in range(zs):
        take_y(s)
        take_core(s)
        if s == 0:
            for i in range(3):
                loads[i].wait()
        experts(s)
        if s + 1 + ahead < zs:
            take_z(s + 1 + ahead)
        if s == 0:
            shared_expert()
        if s >= 2:
            combine(s - 1)
        if s >= 3:
            finish(s - 2)
    if zs > 1:
        combine(zs - 1)
    combine(0)
    for s in range(max(1, zs - 2), zs):
        finish(s)
    finish(0)

    arrived(score_in, co_send.at[zs], co_recv.at[zs], sibling)
    mixed = local_sum[...] + (shared_kept[...] + score_in[...].astype(jnp.float32))
    for s in range(1, zs):
        arrived(z_in.at[zz[s]], zo_send.at[s], zo_recv.at[zz[s]], along[s])
        mixed = mixed + z_in[zz[s]].astype(jnp.float32)
    local_sum[...] = mixed
    squares = jnp.sum(mixed * mixed, axis=1, keepdims=True)
    sq_out[...] = jnp.broadcast_to(squares, sq_out.shape)
    send(sq_out, sq_in, sq_send, sq_recv, sibling)
    arrived(sq_in, sq_send, sq_recv, sibling)
    inverse = lax.rsqrt((squares + sq_in[:, :1]) / width + EPS)
    result_ref[...] = (
        local_sum[...] * inverse * out_gain_ref[...].astype(jnp.float32).reshape(1, half_width)
    ).astype(jnp.bfloat16)
    for copy in sent:
        copy.wait_send()
    for copy, when in passed:
        pl.when(when)(copy.wait_send)


def per_device(tokens, norm_gain, routes, route_weights, gate, up, down, sgate, sup, sdown, out_gain):
    ep = lax.axis_size("ep")
    zs = ep // 2
    rows, width = tokens.shape
    hidden, shidden = gate.shape[2], sgate.shape[1]
    half = width // 2
    bf, f32 = jnp.bfloat16, jnp.float32
    vmem = pl.BlockSpec(memory_space=pltpu.VMEM)
    hbm = pl.BlockSpec(memory_space=pl.ANY)
    dma = pltpu.SemaphoreType.DMA
    flops = 6 * rows * width * (ep * hidden + shidden)
    return pl.pallas_call(
        functools.partial(kernel, ep),
        out_shape=jax.ShapeDtypeStruct((rows, half), bf),
        in_specs=[vmem] * 4 + [hbm] * 6 + [vmem],
        out_specs=vmem,
        scratch_shapes=[
            pltpu.VMEM((ep, rows, width + LANES), bf),
            pltpu.VMEM((width, hidden), bf),
            pltpu.VMEM((width, hidden), bf),
            pltpu.VMEM((hidden, width), bf),
            pltpu.VMEM((width, shidden), bf),
            pltpu.VMEM((width, shidden), bf),
            pltpu.VMEM((shidden, width), bf),
            pltpu.VMEM((zs, 2 * rows, half), f32),
            pltpu.VMEM((rows, half), f32),
            pltpu.VMEM((zs, 2 * rows, half), bf),
            pltpu.VMEM((zs, 2 * rows, half), bf),
            pltpu.VMEM((rows, half), bf),
            pltpu.VMEM((rows, half), bf),
            pltpu.VMEM((zs, rows, half), bf),
            pltpu.VMEM((zs, rows, half), bf),
            pltpu.VMEM((zs, rows, half), bf),
            pltpu.VMEM((zs, rows, half), bf),
            pltpu.VMEM((rows, half), f32),
            pltpu.VMEM((rows, LANES), f32),
            pltpu.VMEM((rows, LANES), f32),
            dma((6,)),
            dma((zs, PIECES)),
            dma((zs, PIECES)),
            dma((zs, PIECES)),
            dma((zs, PIECES)),
            dma((zs, PIECES)),
            dma((zs, PIECES)),
            dma((zs, PIECES)),
            dma((zs, PIECES)),
            dma((zs, PIECES)),
            dma((zs + 1,)),
            dma((zs + 1,)),
            dma((zs,)),
            dma((zs,)),
            dma((zs,)),
            dma((zs,)),
            dma,
            dma,
        ],
        compiler_params=pltpu.CompilerParams(
            collective_id=0, has_side_effects=True, vmem_limit_bytes=60 * 1024 * 1024
        ),
        cost_estimate=pl.CostEstimate(
            flops=flops, bytes_accessed=6 * width * (hidden + shidden), transcendentals=0
        ),
    )(
        tokens,
        norm_gain,
        routes.T,
        route_weights.T,
        gate,
        up,
        down,
        sgate,
        sup,
        sdown,
        out_gain,
    )


def solution(mesh):
    in_specs = (
        P(("grp", "ep"), None),
        P(),
        P(("grp", "ep"), None),
        P(("grp", "ep"), None),
        P("ep", None, "tp"),
        P("ep", None, "tp"),
        P("ep", "tp", None),
        P(None, "tp"),
        P(None, "tp"),
        P("tp", None),
        P("tp"),
    )
    out_specs = P(("grp", "ep"), "tp")
    return jax.shard_map(
        per_device, mesh=mesh, in_specs=in_specs, out_specs=out_specs, check_vma=False
    )
```

```python
import functools

import jax
import jax.numpy as jnp
from jax import lax
from jax.experimental import pallas as pl
from jax.experimental.pallas import tpu as pltpu
from jax.sharding import PartitionSpec as P

EPS = 1e-06
MESH = pl.DeviceIdType.MESH
LANES = 128
HALF_LANES = LANES // 2


PIECES = 2


def by_distance(z, zs):
    table = [sorted(range(zs), key=lambda o: (abs(o - at), -o)) for at in range(zs)]
    order = []
    for k in range(zs):
        pick = table[0][k]
        for at in range(1, zs):
            pick = jnp.where(z == at, table[at][k], pick)
        order.append(pick)
    return order


def kernel(
    ep,
    tokens_ref,
    norm_gain_ref,
    routes_ref,
    weights_ref,
    gate_hbm,
    up_hbm,
    down_hbm,
    sgate_hbm,
    sup_hbm,
    sdown_hbm,
    out_gain_ref,
    result_ref,
    gathered,
    gate,
    up,
    down,
    sgate,
    sup,
    sdown,
    kept,
    shared_kept,
    core_out,
    core_in,
    score_out,
    score_in,
    y_out,
    y_in,
    z_out,
    z_in,
    local_sum,
    sq_out,
    sq_in,
    load_sem,
    r_send,
    l_send,
    z_recv,
    y_send,
    y_recv,
    cz_send,
    cz_recv,
    cy_send,
    cy_recv,
    co_send,
    co_recv,
    yo_send,
    yo_recv,
    zo_send,
    zo_recv,
    sq_send,
    sq_recv,
):
    zs = ep // 2
    rows, width = tokens_ref.shape
    half_rows, half_width = rows // 2, width // 2
    me = lax.axis_index("ep")
    core = lax.axis_index("tp")
    z, y = me // 2, me % 2
    zz = by_distance(z, zs)
    sibling = {"tp": 1 - core}
    across = {"ep": z * 2 + (1 - y)}
    along = [{"ep": zz[s] * 2 + y} for s in range(zs)]

    loads = []
    for i, (src, dst) in enumerate(
        [
            (gate_hbm.at[0], gate),
            (up_hbm.at[0], up),
            (down_hbm.at[0], down),
            (sgate_hbm, sgate),
            (sup_hbm, sup),
            (sdown_hbm, sdown),
        ]
    ):
        copy = pltpu.make_async_copy(src, dst, load_sem.at[i])
        copy.start()
        loads.append(copy)

    barrier = pltpu.get_barrier_semaphore()
    peers = [sibling, across] + along[1:]
    for peer in peers:
        pl.semaphore_signal(barrier, inc=1, device_id=peer, device_id_type=MESH)

    wide = tokens_ref[...].astype(jnp.float32)
    scale = lax.rsqrt(jnp.mean(wide * wide, axis=1, keepdims=True) + EPS)
    gain = norm_gain_ref[...].astype(jnp.float32).reshape(1, width)
    gathered[me, :, :width] = (wide * scale * gain).astype(jnp.bfloat16)
    lane = lax.broadcasted_iota(jnp.int32, (rows, LANES), 1)
    expert = lax.broadcasted_iota(jnp.int32, (LANES, rows), 0) % HALF_LANES
    chosen = jnp.zeros((LANES, rows), jnp.float32)
    for k in range(routes_ref.shape[0]):
        hit = routes_ref[k : k + 1, :] == expert
        chosen = chosen + jnp.where(hit, weights_ref[k : k + 1, :], 0.0)
    chosen = chosen.T
    high = chosen.astype(jnp.bfloat16).astype(jnp.float32)
    gathered[me, :, width:] = jnp.where(lane < HALF_LANES, high, chosen - high).astype(
        jnp.bfloat16
    )

    pl.semaphore_wait(barrier, len(peers))

    piece = half_rows // PIECES

    def rows_of(which, q):
        return pl.ds(pl.multiple_of(which * half_rows + q * piece, piece), piece)

    my_cols = pl.ds(pl.multiple_of(core * half_width, half_width), half_width)
    other_cols = pl.ds(pl.multiple_of((1 - core) * half_width, half_width), half_width)

    sent = []

    def send(src, dst, send_sem, recv_sem, target):
        copy = pltpu.make_async_remote_copy(
            src_ref=src,
            dst_ref=dst,
            send_sem=send_sem,
            recv_sem=recv_sem,
            device_id=target,
            device_id_type=MESH,
        )
        copy.start()
        sent.append(copy)
        return copy

    def arrived(ref, send_sem, recv_sem, target):
        pltpu.make_async_remote_copy(
            src_ref=ref,
            dst_ref=ref,
            send_sem=send_sem,
            recv_sem=recv_sem,
            device_id=target,
            device_id_type=MESH,
        ).wait_recv()

    passed = []

    def make_pass(block, q, source, sends, target, when):
        copy = pltpu.make_async_remote_copy(
            src_ref=block,
            dst_ref=block,
            send_sem=sends.at[source, q],
            recv_sem=z_recv.at[source, q],
            device_id={"ep": target * 2 + y},
            device_id_type=MESH,
        )
        passed.append((copy, when))
        return copy, when

    for q in range(PIECES):
        own = gathered.at[me, rows_of(core, q)]
        for copy, when in (
            make_pass(own, q, z, r_send, z + 1, z < zs - 1),
            make_pass(own, q, z, l_send, z - 1, z > 0),
        ):
            pl.when(when)(copy.start)
        send(own, own, y_send.at[0, q], y_recv.at[0, q], across)

    def make(src, dst, send_sem, recv_sem, target):
        return pltpu.make_async_remote_copy(
            src_ref=src,
            dst_ref=dst,
            send_sem=send_sem,
            recv_sem=recv_sem,
            device_id=target,
            device_id_type=MESH,
        )

    steps = {}
    for s in range(1, zs):
        steps[s] = []
        for q in range(PIECES):
            block = gathered.at[zz[s] * 2 + y, rows_of(core, q)]
            right = jnp.logical_and(zz[s] < z, z < zs - 1)
            left = jnp.logical_and(zz[s] > z, z > 0)
            passes = [
                make_pass(block, q, zz[s], r_send, z + 1, right),
                make_pass(block, q, zz[s], l_send, z - 1, left),
            ]
            coming = make(block, block, r_send.at[zz[s], q], z_recv.at[zz[s], q], across)
            going = [
                make(block, block, y_send.at[s, q], y_recv.at[s, q], across),
                make(block, block, cz_send.at[s, q], cz_recv.at[s, q], sibling),
            ]
            sent.extend(going)
            steps[s].append((coming, passes, going))

    def take_z(s, where=None):
        def body():
            for coming, passes, going in steps[s]:
                coming.wait_recv()
                for copy, when in passes:
                    pl.when(when)(copy.start)
                for copy in going:
                    copy.start()

        if s < zs:
            body() if where is None else pl.when(where)(body)

    def take_y(s):
        for q in range(PIECES):
            block = gathered.at[zz[s] * 2 + (1 - y), rows_of(core, q)]
            arrived(block, y_send.at[s, q], y_recv.at[s, q], across)
            send(block, block, cy_send.at[s, q], cy_recv.at[s, q], sibling)

    def take_core(s):
        for q in range(PIECES):
            if s > 0:
                block = gathered.at[zz[s] * 2 + y, rows_of(1 - core, q)]
                arrived(block, cz_send.at[s, q], cz_recv.at[s, q], sibling)
            block = gathered.at[zz[s] * 2 + (1 - y), rows_of(1 - core, q)]
            arrived(block, cy_send.at[s, q], cy_recv.at[s, q], sibling)

    def swiglu(x, gate_w, up_w):
        g = jnp.dot(x, gate_w[...], preferred_element_type=jnp.float32)
        u = jnp.dot(x, up_w[...], preferred_element_type=jnp.float32)
        return (g / (1.0 + jnp.exp(-g)) * u).astype(jnp.bfloat16)

    def experts(s):
        pair = gathered.at[pl.ds(zz[s] * 2, 2)]
        x = pair[:, :, :width].reshape(2 * rows, width)
        act = swiglu(x, gate, up)
        core_out[s] = jnp.dot(
            act, down[:, other_cols], preferred_element_type=jnp.float32
        ).astype(jnp.bfloat16)
        send(core_out.at[s], core_in.at[s], co_send.at[s], co_recv.at[s], sibling)
        kept[s] = jnp.dot(act, down[:, my_cols], preferred_element_type=jnp.float32)

    def weight_of(block):
        spread = gathered[block, :, width:].astype(jnp.float32)
        return jnp.sum(
            jnp.where(lane % HALF_LANES == me, spread, 0.0), axis=1, keepdims=True
        )

    def combine(s):
        arrived(core_in.at[s], co_send.at[s], co_recv.at[s], sibling)
        theirs = pl.ds(pl.multiple_of((1 - y) * rows, rows), rows)
        value = kept[s, theirs] + core_in[s, theirs].astype(jnp.float32)
        y_out[s] = (value * weight_of(zz[s] * 2 + (1 - y))).astype(jnp.bfloat16)
        send(y_out.at[s], y_in.at[s], yo_send.at[s], yo_recv.at[s], across)

    def finish(s):
        mine = pl.ds(pl.multiple_of(y * rows, rows), rows)
        value = kept[s, mine] + core_in[s, mine].astype(jnp.float32)
        value = value * weight_of(zz[s] * 2 + y)
        arrived(y_in.at[s], yo_send.at[s], yo_recv.at[s], across)
        value = value + y_in[s].astype(jnp.float32)
        if s == 0:
            local_sum[...] = value
        else:
            z_out[s] = value.astype(jnp.bfloat16)
            send(z_out.at[s], z_in.at[z], zo_send.at[s], zo_recv.at[z], along[s])

    def shared_expert():
        for i in range(3, 6):
            loads[i].wait()
        act = swiglu(gathered[me, :, :width], sgate, sup)
        score_out[...] = jnp.dot(
            act, sdown[:, other_cols], preferred_element_type=jnp.float32
        ).astype(jnp.bfloat16)
        send(score_out, score_in, co_send.at[zs], co_recv.at[zs], sibling)
        shared_kept[...] = jnp.dot(act, sdown[:, my_cols], preferred_element_type=jnp.float32)

    end = jnp.logical_or(z == 0, z == zs - 1)
    inner = jnp.logical_and(z > 0, z < zs - 1)
    take_z(1)
    take_z(2, inner)
    for s in range(zs):
        take_y(s)
        take_core(s)
        if s == 0:
            for i in range(3):
                loads[i].wait()
        experts(s)
        take_z(s + 3, inner)
        if s == 0:
            shared_expert()
        take_z(s + 2, end)
        if 1 <= s < zs - 1:
            combine(s)
        if s >= 2:
            finish(s - 1)
    if zs > 1:
        combine(zs - 1)
    combine(0)
    for s in range(max(1, zs - 1), zs):
        finish(s)
    finish(0)

    arrived(score_in, co_send.at[zs], co_recv.at[zs], sibling)
    mixed = local_sum[...] + (shared_kept[...] + score_in[...].astype(jnp.float32))
    for s in range(1, zs):
        arrived(z_in.at[zz[s]], zo_send.at[s], zo_recv.at[zz[s]], along[s])
        mixed = mixed + z_in[zz[s]].astype(jnp.float32)
    local_sum[...] = mixed
    squares = jnp.sum(mixed * mixed, axis=1, keepdims=True)
    sq_out[...] = jnp.broadcast_to(squares, sq_out.shape)
    send(sq_out, sq_in, sq_send, sq_recv, sibling)
    arrived(sq_in, sq_send, sq_recv, sibling)
    inverse = lax.rsqrt((squares + sq_in[:, :1]) / width + EPS)
    result_ref[...] = (
        local_sum[...] * inverse * out_gain_ref[...].astype(jnp.float32).reshape(1, half_width)
    ).astype(jnp.bfloat16)
    for copy in sent:
        copy.wait_send()
    for copy, when in passed:
        pl.when(when)(copy.wait_send)


def per_device(tokens, norm_gain, routes, route_weights, gate, up, down, sgate, sup, sdown, out_gain):
    ep = lax.axis_size("ep")
    zs = ep // 2
    rows, width = tokens.shape
    hidden, shidden = gate.shape[2], sgate.shape[1]
    half = width // 2
    bf, f32 = jnp.bfloat16, jnp.float32
    vmem = pl.BlockSpec(memory_space=pltpu.VMEM)
    hbm = pl.BlockSpec(memory_space=pl.ANY)
    dma = pltpu.SemaphoreType.DMA
    flops = 6 * rows * width * (ep * hidden + shidden)
    return pl.pallas_call(
        functools.partial(kernel, ep),
        out_shape=jax.ShapeDtypeStruct((rows, half), bf),
        in_specs=[vmem] * 4 + [hbm] * 6 + [vmem],
        out_specs=vmem,
        scratch_shapes=[
            pltpu.VMEM((ep, rows, width + LANES), bf),
            pltpu.VMEM((width, hidden), bf),
            pltpu.VMEM((width, hidden), bf),
            pltpu.VMEM((hidden, width), bf),
            pltpu.VMEM((width, shidden), bf),
            pltpu.VMEM((width, shidden), bf),
            pltpu.VMEM((shidden, width), bf),
            pltpu.VMEM((zs, 2 * rows, half), f32),
            pltpu.VMEM((rows, half), f32),
            pltpu.VMEM((zs, 2 * rows, half), bf),
            pltpu.VMEM((zs, 2 * rows, half), bf),
            pltpu.VMEM((rows, half), bf),
            pltpu.VMEM((rows, half), bf),
            pltpu.VMEM((zs, rows, half), bf),
            pltpu.VMEM((zs, rows, half), bf),
            pltpu.VMEM((zs, rows, half), bf),
            pltpu.VMEM((zs, rows, half), bf),
            pltpu.VMEM((rows, half), f32),
            pltpu.VMEM((rows, LANES), f32),
            pltpu.VMEM((rows, LANES), f32),
            dma((6,)),
            dma((zs, PIECES)),
            dma((zs, PIECES)),
            dma((zs, PIECES)),
            dma((zs, PIECES)),
            dma((zs, PIECES)),
            dma((zs, PIECES)),
            dma((zs, PIECES)),
            dma((zs, PIECES)),
            dma((zs, PIECES)),
            dma((zs + 1,)),
            dma((zs + 1,)),
            dma((zs,)),
            dma((zs,)),
            dma((zs,)),
            dma((zs,)),
            dma,
            dma,
        ],
        compiler_params=pltpu.CompilerParams(
            collective_id=0, has_side_effects=True, vmem_limit_bytes=60 * 1024 * 1024
        ),
        cost_estimate=pl.CostEstimate(
            flops=flops, bytes_accessed=6 * width * (hidden + shidden), transcendentals=0
        ),
    )(
        tokens,
        norm_gain,
        routes.T,
        route_weights.T,
        gate,
        up,
        down,
        sgate,
        sup,
        sdown,
        out_gain,
    )


def solution(mesh):
    in_specs = (
        P(("grp", "ep"), None),
        P(),
        P(("grp", "ep"), None),
        P(("grp", "ep"), None),
        P("ep", None, "tp"),
        P("ep", None, "tp"),
        P("ep", "tp", None),
        P(None, "tp"),
        P(None, "tp"),
        P("tp", None),
        P("tp"),
    )
    out_specs = P(("grp", "ep"), "tp")
    return jax.shard_map(
        per_device, mesh=mesh, in_specs=in_specs, out_specs=out_specs, check_vma=False
    )
```
